32 devices in a mesh: ra: 4 (over y, x), cb: 8 (over z, core).
Axes of the slice: x: 2, y: 2, z: 4, core: 2. Of those that a mesh axis runs over, the one named last changes fastest.
Arguments:
- tokens: bfloat16 [512, 4096], P(None, 'ra'), may hold values from -40 to 40, as said below
- norm_gain: float32 [2, 4096], P(None, 'ra'), may hold values from 0.1 to 1.9
- gate_weight: bfloat16 [2, 4096, 11264], P(None, 'ra', 'cb'), may hold values from -0.09375 to 0.09375
- up_weight: bfloat16 [2, 4096, 11264], P(None, 'ra', 'cb'), may hold values from -0.09375 to 0.09375
- down_weight: bfloat16 [2, 11264, 4096], P(None, 'cb', 'ra'), may hold values from -0.0546875 to 0.0546875
Outputs:
- result: bfloat16 [512, 4096], P(None, 'ra')
The draws below stay inside these ranges and needn't reach their ends.
Inputs may be any that keep to these rules, and one draw needn't show every extreme that they name: `tokens`: features come in blocks of 32 with scales that differ from block to block by up to a factor of 16.
All inputs are finite; a program needn't handle non-finite values.
Results may differ from the reference program's by a relative error of at most 0.0075.
Values may be sent and summed in bfloat16 or wider, within the bound.
A program may use at most 64 MiB of HBM per device.

```python
import jax
import jax.numpy as jnp
from jax import lax

D = 4096
FF = 11264
TOKENS = 512
LAYERS = 2


def draw_tokens(key, part):
    first, second, third = jax.random.split(key, 3)
    base = jax.random.normal(first, (TOKENS, D), jnp.float32)
    blocks = jax.random.uniform(second, (D // 32,), jnp.float32, -1.0, 1.0)
    factor = jnp.repeat(4.0 ** blocks, 32)
    values = base * factor
    return jnp.clip(values, -40.0, 40.0).astype(jnp.bfloat16)


def levels(rng, extent, cuts, low, largest):
    def one(dim, shards_of):
        heights = jax.random.uniform(jax.random.fold_in(jax.random.fold_in(rng, 6), dim), (shards_of,), jnp.float32, low / len(cuts), largest / len(cuts))
        return jnp.repeat(jnp.exp(heights), extent[dim] // shards_of).reshape((-1,) + (1,) * (len(extent) - dim - 1))

    level = one(*cuts[0])
    for cut in cuts[1:]:
        level = level * one(*cut)
    return level


def normal_values(key, shape, deviation, limit, cuts=(), kind=jnp.bfloat16):
    factor_of = levels(key, shape, cuts, -0.22, 0.18) if cuts else 1.0
    values = jax.random.normal(key, shape, jnp.float32) * deviation * factor_of
    return jnp.minimum(jnp.maximum(values, -limit), limit).astype(kind)


def setup_inputs(seed: int = 0) -> dict:
    seeds = jax.random.split(jax.random.key(seed), 6)
    tokens = draw_tokens(jax.random.fold_in(seeds[5], 71), 0)
    norm_gain = jnp.clip(1.0 + 0.18 * jax.random.normal(seeds[1], (LAYERS, D), jnp.float32), 0.1, 1.9)
    gate_weight = normal_values(seeds[2], (LAYERS, D, FF), D ** -0.5, 0.09375, ((1, 4), (2, 8)))
    up_weight = normal_values(seeds[3], (LAYERS, D, FF), D ** -0.5, 0.09375, ((1, 4), (2, 8)))
    down_weight = normal_values(seeds[4], (LAYERS, FF, D), FF ** -0.5, 0.0546875, ((1, 8), (2, 4)))
    return {"tokens": tokens, "norm_gain": norm_gain, "gate_weight": gate_weight, "up_weight": up_weight, "down_weight": down_weight}


epsilon = 1e-06
keep_share = 0.5

def sublayer(stream, gain, gate_w, up_w, down_w):
    widened = stream.astype(jnp.float32)
    scale = lax.rsqrt(lax.optimization_barrier(jnp.mean(widened * widened, axis=-1, keepdims=True)) + epsilon)
    normed = (widened * gain).astype(jnp.bfloat16)
    gate = jnp.dot(normed, gate_w, preferred_element_type=jnp.float32) * scale
    up_val = jnp.dot(normed, up_w, preferred_element_type=jnp.float32) * scale
    hidden = (jax.nn.silu(gate) * up_val).astype(jnp.bfloat16)
    branch = jnp.dot(hidden, down_w, preferred_element_type=jnp.float32)
    return (keep_share * widened + branch).astype(jnp.bfloat16)

def reference(tokens, norm_gain, gate_weight, up_weight, down_weight):
    stream = tokens
    for layer in range(LAYERS):
        stream = sublayer(stream, norm_gain[layer], gate_weight[layer], up_weight[layer], down_weight[layer])
    return stream
```

```python
import functools
import math

import jax
import jax.numpy as jnp
from jax import lax
from jax.experimental import pallas as pl
from jax.experimental.pallas import tpu as pltpu
from jax.sharding import PartitionSpec as P

MESH = pl.DeviceIdType.MESH
EPSILON = 1e-06
KEEP_SHARE = 0.5
DEPTH = 4
F32 = jnp.float32
BF16 = jnp.bfloat16


def column_tiles(width, tile, visit):
    for start in range(0, width, tile):
        visit(start, min(tile, width - start))


def kernel(cfg, tok, gain, wg_hbm, up_hbm, wd_hbm, out,
           stream, wg, wu, wd, gbuf, ubuf, r1g, r1u, s1g, s1u, r2g, r2u, ssl, ssr,
           hid, pbuf, crecv, cs, zr, wsem, tsem, osem, ssem, rsem):
    nx, ny, nz, layers, chunks, features = (cfg[n] for n in ("nx", "ny", "nz", "layers", "chunks", "features"))
    nra = nx * ny
    period = max(chunks, DEPTH)
    r = lax.axis_index("ra")
    b = lax.axis_index("cb")
    x0, y0 = lax.rem(r, nx), lax.div(r, nx)
    core, z0 = lax.rem(b, 2), lax.div(b, 2)
    rw, ff = gbuf.shape[3], gbuf.shape[4]
    half = rw // 2
    tc = nra * rw
    dl = stream.shape[-1]
    rz = stream.shape[4]

    def load_w(layer, which):
        src, dst = ((wg_hbm, wg), (up_hbm, wu), (wd_hbm, wd))[which]
        return pltpu.make_async_copy(src.at[layer], dst.at[layer], wsem.at[layer, which])

    tokens_in = pltpu.make_async_copy(tok, stream.at[0], tsem.at[0])
    tokens_in.start()
    for layer in range(layers):
        for which in range(3):
            load_w(layer, which).start()

    barrier = pltpu.get_barrier_semaphore()
    for d in range(1, nra):
        pl.semaphore_signal(barrier, inc=1, device_id={"ra": lax.rem(r + d, nra)}, device_id_type=MESH)
    for d in range(1, nz):
        pl.semaphore_signal(barrier, inc=1, device_id={"cb": lax.rem(z0 + d, nz) * 2 + core}, device_id_type=MESH)
    pl.semaphore_signal(barrier, inc=1, device_id={"cb": z0 * 2 + 1 - core}, device_id_type=MESH)
    pl.semaphore_wait(barrier, nra + nz - 1)

    base = {}
    at = 0
    for name, count in cfg["kinds"]:
        base[name] = at
        at += count

    def remote(k, name, i, src, dst, device):
        return pltpu.make_async_remote_copy(
            src_ref=src, dst_ref=dst, send_sem=ssem.at[k, base[name] + i], recv_sem=rsem.at[k, base[name] + i],
            device_id=device, device_id_type=MESH)

    def to_x(d):
        xp = lax.rem(x0 + d, nx)
        return xp, {"ra": y0 * nx + xp}

    def to_y(d):
        yp = lax.rem(y0 + d, ny)
        return yp, {"ra": yp * nx + x0}

    def to_z(d):
        zp = lax.rem(z0 + d, nz)
        return zp, {"cb": zp * 2 + core}

    partner = {"cb": z0 * 2 + 1 - core}

    def copies(name, layer, c):
        k = layer * chunks + c
        made = []
        if name == "g1":
            for d in range(1, nx):
                xp, dev = to_x(d)
                made.append(remote(k, name, d - 1, gbuf.at[k, :, xp], r1g.at[k, d - 1], dev))
        if name == "u1":
            for d in range(1, ny):
                yp, dev = to_y(d)
                made.append(remote(k, name, d - 1, ubuf.at[k, yp], r1u.at[k, d - 1], dev))
        if name == "ss":
            for d in range(1, nra):
                made.append(remote(k, name, d - 1, ssl.at[k], ssr.at[k, d - 1], {"ra": lax.rem(r + d, nra)}))
        if name == "g2":
            for d in range(1, ny):
                yp, dev = to_y(d)
                made.append(remote(k, name, d - 1, s1g.at[k, yp], r2g.at[k, d - 1], dev))
        if name == "u2":
            for d in range(1, nx):
                xp, dev = to_x(d)
                made.append(remote(k, name, d - 1, s1u.at[k, xp], r2u.at[k, d - 1], dev))
        if name == "a1":
            for d in range(1, nx):
                part = hid.at[k, y0, x0, pl.ds(0, half)]
                made.append(remote(k, name, d - 1, part, part, to_x(d)[1]))
            for d in range(1, ny):
                part = hid.at[k, y0, x0, pl.ds(half, half)]
                made.append(remote(k, name, nx - 1 + d - 1, part, part, to_y(d)[1]))
        if name == "a2":
            for d in range(1, ny):
                part = hid.at[k, y0, :, pl.ds(0, half)]
                made.append(remote(k, name, d - 1, part, part, to_y(d)[1]))
            for d in range(1, nx):
                part = hid.at[k, :, x0, pl.ds(half, half)]
                made.append(remote(k, name, ny - 1 + d - 1, part, part, to_x(d)[1]))
        if name == "c1":
            made.append(remote(k, name, 0, pbuf.at[k, 1 - core], crecv.at[k], partner))
        if name == "z1":
            for d in range(1, nz):
                zp, dev = to_z(d)
                made.append(remote(k, name, d - 1, cs.at[k, zp], zr.at[k, d - 1], dev))
        if name == "z2":
            for d in range(1, nz):
                part = stream.at[layer + 1, c, core, z0]
                made.append(remote(k, name, d - 1, part, part, to_z(d)[1]))
        if name == "c2":
            part = stream.at[layer + 1, c, core]
            made.append(remote(k, name, 0, part, part, partner))
        return made

    def start(name, layer, c):
        for copy in copies(name, layer, c):
            copy.start()

    def arrived(name, layer, c):
        for copy in copies(name, layer, c):
            copy.wait_recv()

    def stage0(layer, c):
        k = layer * chunks + c

        @pl.when((layer == 0) & (c == 0))
        def _():
            tokens_in.wait()

        @pl.when(layer > 0)
        def _():
            arrived("c2", layer - 1, c)

        @pl.when(c == 0)
        def _():
            load_w(layer, 0).wait()
            load_w(layer, 1).wait()

        wide = stream[layer, c].reshape(tc, dl).astype(F32)
        normed = (wide * gain[layer]).astype(BF16)

        def gate_tile(s, w):
            part = jnp.dot(normed, wg[layer, :, s:s + w], preferred_element_type=F32)
            gbuf[k, :, :, :, s:s + w] = part.astype(BF16).reshape(ny, nx, rw, w)

        def up_tile(s, w):
            part = jnp.dot(normed, wu[layer, :, s:s + w], preferred_element_type=F32)
            ubuf[k, :, :, :, s:s + w] = part.astype(BF16).reshape(ny, nx, rw, w)

        column_tiles(ff, 512, gate_tile)
        start("g1", layer, c)
        column_tiles(ff, 512, up_tile)
        start("u1", layer, c)
        column = jnp.sum(wide * wide, axis=1, keepdims=True)
        diagonal = lax.broadcasted_iota(jnp.int32, (tc, tc), 0) == lax.broadcasted_iota(jnp.int32, (tc, tc), 1)
        ssl[k] = jnp.broadcast_to(jnp.sum(jnp.where(diagonal, column, 0.0), axis=0, keepdims=True), (8, tc))
        start("ss", layer, c)

    def stage1(layer, c):
        k = layer * chunks + c
        arrived("g1", layer, c)
        total = gbuf[k, :, x0].astype(F32)
        for d in range(nx - 1):
            total = total + r1g[k, d].astype(F32)
        s1g[k] = total.astype(BF16)
        start("g2", layer, c)
        arrived("u1", layer, c)
        total = ubuf[k, y0].astype(F32)
        for d in range(ny - 1):
            total = total + r1u[k, d].astype(F32)
        s1u[k] = total.astype(BF16)
        start("u2", layer, c)

    def stage2(layer, c):
        k = layer * chunks + c
        arrived("ss", layer, c)
        squares = ssl[k, 0:1]
        for d in range(nra - 1):
            squares = squares + ssr[k, d, 0:1]
        mine = lax.broadcasted_iota(jnp.int32, (rw, tc), 0) + r * rw == lax.broadcasted_iota(jnp.int32, (rw, tc), 1)
        column = jnp.sum(jnp.where(mine, squares, 0.0), axis=1, keepdims=True)
        scale = lax.rsqrt(column / features + EPSILON)
        arrived("g2", layer, c)
        arrived("u2", layer, c)
        gate = s1g[k, y0].astype(F32)
        for d in range(ny - 1):
            gate = gate + r2g[k, d].astype(F32)
        up = s1u[k, x0].astype(F32)
        for d in range(nx - 1):
            up = up + r2u[k, d].astype(F32)
        hid[k, y0, x0] = (jax.nn.silu(gate * scale) * (up * scale)).astype(BF16)
        start("a1", layer, c)

    def stage3(layer, c):
        arrived("a1", layer, c)
        start("a2", layer, c)

    def stage4(layer, c):
        k = layer * chunks + c
        arrived("a2", layer, c)

        @pl.when(c == 0)
        def _():
            load_w(layer, 2).wait()

        full = hid[k].reshape(tc, ff)

        def down_tile(s, w):
            part = jnp.dot(full, wd[layer, :, s:s + w], preferred_element_type=F32)
            pbuf[k, :, :, :, s:s + w] = part.astype(BF16).reshape(2, nz, rz, w)

        column_tiles(dl, 512, down_tile)
        start("c1", layer, c)

    def stage5(layer, c):
        k = layer * chunks + c
        arrived("c1", layer, c)
        cs[k] = (pbuf[k, core].astype(F32) + crecv[k].astype(F32)).astype(BF16)
        start("z1", layer, c)

    def stage6(layer, c):
        k = layer * chunks + c
        arrived("z1", layer, c)
        branch = cs[k, z0].astype(F32)
        for d in range(nz - 1):
            branch = branch + zr[k, d].astype(F32)
        kept = stream[layer, c, core, z0].astype(F32)
        stream[layer + 1, c, core, z0] = (KEEP_SHARE * kept + branch).astype(BF16)
        start("z2", layer, c)

    def stage7(layer, c):
        arrived("z2", layer, c)
        start("c2", layer, c)

    def write_out(c):
        return pltpu.make_async_copy(stream.at[layers, c], out.at[c], osem.at[c])

    def stage8(layer, c):
        @pl.when(layer == layers - 1)
        def _():
            arrived("c2", layer, c)
            write_out(c).start()

    def run(stage, u, offset):
        v = u - offset
        layer, c = lax.div(v, period), lax.rem(v, period)

        @pl.when((v >= 0) & (layer < layers) & (c < chunks))
        def _():
            stage(layer, c)

    def step(u, carry):
        for stage, offset in cfg["order"]:
            run((stage0, stage1, stage2, stage3, stage4, stage5, stage6, stage7, stage8)[stage], u, offset)
        return carry

    lax.fori_loop(0, layers * period + DEPTH, step, 0)

    def finish(k, carry):
        layer, c = lax.div(k, chunks), lax.rem(k, chunks)
        for name, _ in cfg["kinds"]:
            for copy in copies(name, layer, c):
                copy.wait_send()
        return carry

    lax.fori_loop(0, layers * chunks, finish, 0)
    for c in range(chunks):
        write_out(c).wait()


ORDER = ((0, 0), (2, 1), (4, 2), (6, 3), (8, 4), (1, 0), (3, 1), (5, 2), (7, 3))


def solution(mesh):
    nra, ncb = mesh.shape["ra"], mesh.shape["cb"]
    ny = max(d for d in range(1, math.isqrt(nra) + 1) if nra % d == 0)
    nx = nra // ny
    nz = ncb // 2

    def body(tokens, norm_gain, gate_weight, up_weight, down_weight):
        rows, dl = tokens.shape
        layers, _, ff = gate_weight.shape
        tc = min(rows, max(32 * nra, 16 * ncb))
        chunks = rows // tc
        rw, rz = tc // nra, tc // ncb
        items = layers * chunks
        kinds = (("g1", nx - 1), ("u1", ny - 1), ("ss", nra - 1), ("g2", ny - 1), ("u2", nx - 1),
                 ("a1", nx + ny - 2), ("a2", nx + ny - 2), ("c1", 1), ("z1", nz - 1), ("z2", nz - 1), ("c2", 1))
        sems = sum(n for _, n in kinds)
        cfg = dict(nx=nx, ny=ny, nz=nz, layers=layers, chunks=chunks, features=dl * nra, kinds=kinds, order=ORDER)
        hbm = pl.BlockSpec(memory_space=pl.ANY)
        vmem = pl.BlockSpec(memory_space=pltpu.VMEM)
        shaped = (chunks, 2, nz, rz, dl)
        result = pl.pallas_call(
            functools.partial(kernel, cfg),
            out_shape=jax.ShapeDtypeStruct(shaped, BF16),
            in_specs=[hbm, vmem, hbm, hbm, hbm],
            out_specs=hbm,
            scratch_shapes=[
                pltpu.VMEM((layers + 1,) + shaped, BF16),
                pltpu.VMEM((layers, dl, ff), BF16),
                pltpu.VMEM((layers, dl, ff), BF16),
                pltpu.VMEM((layers, ff, dl), BF16),
                pltpu.VMEM((items, ny, nx, rw, ff), BF16),
                pltpu.VMEM((items, ny, nx, rw, ff), BF16),
                pltpu.VMEM((items, nx - 1, ny, rw, ff), BF16),
                pltpu.VMEM((items, ny - 1, nx, rw, ff), BF16),
                pltpu.VMEM((items, ny, rw, ff), BF16),
                pltpu.VMEM((items, nx, rw, ff), BF16),
                pltpu.VMEM((items, ny - 1, rw, ff), BF16),
                pltpu.VMEM((items, nx - 1, rw, ff), BF16),
                pltpu.VMEM((items, 8, tc), F32),
                pltpu.VMEM((items, nra - 1, 8, tc), F32),
                pltpu.VMEM((items, ny, nx, rw, ff), BF16),
                pltpu.VMEM((items, 2, nz, rz, dl), BF16),
                pltpu.VMEM((items, nz, rz, dl), BF16),
                pltpu.VMEM((items, nz, rz, dl), BF16),
                pltpu.VMEM((items, nz - 1, rz, dl), BF16),
                pltpu.SemaphoreType.DMA((layers, 3)),
                pltpu.SemaphoreType.DMA((1,)),
                pltpu.SemaphoreType.DMA((chunks,)),
                pltpu.SemaphoreType.DMA((items, sems)),
                pltpu.SemaphoreType.DMA((items, sems)),
            ],
            compiler_params=pltpu.CompilerParams(
                collective_id=0, has_side_effects=True, vmem_limit_bytes=67_043_328),
            name="sublayers",
        )(tokens.reshape(shaped), norm_gain.reshape(layers, 1, dl), gate_weight, up_weight, down_weight)
        return result.reshape(rows, dl)

    placed = (
        P(None, "ra"),
        P(None, "ra"),
        P(None, "ra", "cb"),
        P(None, "ra", "cb"),
        P(None, "cb", "ra"),
    )
    return jax.shard_map(body, mesh=mesh, in_specs=placed, out_specs=P(None, "ra"), check_vma=False)
```

```python
import functools
import math

import jax
import jax.numpy as jnp
from jax import lax
from jax.experimental import pallas as pl
from jax.experimental.pallas import tpu as pltpu
from jax.sharding import PartitionSpec as P

MESH = pl.DeviceIdType.MESH
EPSILON = 1e-06
KEEP_SHARE = 0.5
DEPTH = 4
F32 = jnp.float32
BF16 = jnp.bfloat16


def column_tiles(width, tile, visit):
    for start in range(0, width, tile):
        visit(start, min(tile, width - start))


def kernel(cfg, tok, gain, wg_hbm, up_hbm, wd_hbm, out,
           stream, wg, wu, wd, gbuf, ubuf, r1g, r1u, s1g, s1u, r2g, r2u, ssl, ssr,
           gown, uown, s1gown, s1uown, pown, csown, hid, pbuf, crecv, cs, zr, wsem, tsem, osem, ssem, rsem):
    nx, ny, nz, layers, chunks, features = (cfg[n] for n in ("nx", "ny", "nz", "layers", "chunks", "features"))
    nra = nx * ny
    period = max(chunks, DEPTH)
    r = lax.axis_index("ra")
    b = lax.axis_index("cb")
    x0, y0 = lax.rem(r, nx), lax.div(r, nx)
    core, z0 = lax.rem(b, 2), lax.div(b, 2)
    rw, ff = gbuf.shape[3], gbuf.shape[4]
    half = rw // 2
    tc = nra * rw
    dl = stream.shape[-1]
    rz = stream.shape[4]

    def load_w(layer, which):
        src, dst = ((wg_hbm, wg), (up_hbm, wu), (wd_hbm, wd))[which]
        return pltpu.make_async_copy(src.at[layer], dst.at[layer], wsem.at[layer, which])

    tokens_in = pltpu.make_async_copy(tok, stream.at[0], tsem.at[0])
    tokens_in.start()
    load_w(0, 0).start()
    load_w(0, 1).start()

    barrier = pltpu.get_barrier_semaphore()
    for d in range(1, nra):
        pl.semaphore_signal(barrier, inc=1, device_id={"ra": lax.rem(r + d, nra)}, device_id_type=MESH)
    for d in range(1, nz):
        pl.semaphore_signal(barrier, inc=1, device_id={"cb": lax.rem(z0 + d, nz) * 2 + core}, device_id_type=MESH)
    pl.semaphore_signal(barrier, inc=1, device_id={"cb": z0 * 2 + 1 - core}, device_id_type=MESH)
    pl.semaphore_wait(barrier, nra + nz - 1)

    base = {}
    at = 0
    for name, count in cfg["kinds"]:
        base[name] = at
        at += count

    def remote(k, name, i, src, dst, device):
        return pltpu.make_async_remote_copy(
            src_ref=src, dst_ref=dst, send_sem=ssem.at[k, base[name] + i], recv_sem=rsem.at[k, base[name] + i],
            device_id=device, device_id_type=MESH)

    def to_x(d):
        xp = lax.rem(x0 + d, nx)
        return xp, {"ra": y0 * nx + xp}

    def to_y(d):
        yp = lax.rem(y0 + d, ny)
        return yp, {"ra": yp * nx + x0}

    def to_z(d):
        zp = lax.rem(z0 + d, nz)
        return zp, {"cb": zp * 2 + core}

    partner = {"cb": z0 * 2 + 1 - core}

    def copies(name, layer, c):
        k = layer * chunks + c
        made = []
        if name == "g1":
            for d in range(1, nx):
                xp, dev = to_x(d)
                made.append(remote(k, name, d - 1, gbuf.at[k, :, xp], r1g.at[k, d - 1], dev))
        if name == "u1":
            for d in range(1, ny):
                yp, dev = to_y(d)
                made.append(remote(k, name, d - 1, ubuf.at[k, yp], r1u.at[k, d - 1], dev))
        if name == "ss":
            for d in range(1, nra):
                made.append(remote(k, name, d - 1, ssl.at[k], ssr.at[k, d - 1], {"ra": lax.rem(r + d, nra)}))
        if name == "g2":
            for d in range(1, ny):
                yp, dev = to_y(d)
                made.append(remote(k, name, d - 1, s1g.at[k, yp], r2g.at[k, d - 1], dev))
        if name == "u2":
            for d in range(1, nx):
                xp, dev = to_x(d)
                made.append(remote(k, name, d - 1, s1u.at[k, xp], r2u.at[k, d - 1], dev))
        if name == "a1":
            for d in range(1, nx):
                part = hid.at[k, y0, x0, pl.ds(0, half)]
                made.append(remote(k, name, d - 1, part, part, to_x(d)[1]))
            for d in range(1, ny):
                part = hid.at[k, y0, x0, pl.ds(half, half)]
                made.append(remote(k, name, nx - 1 + d - 1, part, part, to_y(d)[1]))
        if name == "a2":
            for d in range(1, ny):
                part = hid.at[k, y0, :, pl.ds(0, half)]
                made.append(remote(k, name, d - 1, part, part, to_y(d)[1]))
            for d in range(1, nx):
                part = hid.at[k, :, x0, pl.ds(half, half)]
                made.append(remote(k, name, ny - 1 + d - 1, part, part, to_x(d)[1]))
        if name == "c1":
            made.append(remote(k, name, 0, pbuf.at[k, 1 - core], crecv.at[k], partner))
        if name == "z1":
            for d in range(1, nz):
                zp, dev = to_z(d)
                made.append(remote(k, name, d - 1, cs.at[k, zp], zr.at[k, d - 1], dev))
        if name == "z2":
            for d in range(1, nz):
                part = stream.at[layer + 1, c, core, z0]
                made.append(remote(k, name, d - 1, part, part, to_z(d)[1]))
        if name == "c2":
            part = stream.at[layer + 1, c, core]
            made.append(remote(k, name, 0, part, part, partner))
        return made

    def start(name, layer, c):
        for copy in copies(name, layer, c):
            copy.start()

    def arrived(name, layer, c):
        for copy in copies(name, layer, c):
            copy.wait_recv()

    def stage0(layer, c):
        k = layer * chunks + c

        @pl.when((layer == 0) & (c == 0))
        def _():
            tokens_in.wait()

        @pl.when(layer > 0)
        def _():
            arrived("c2", layer - 1, c)

        @pl.when(c == 0)
        def _():
            load_w(layer, 0).wait()

        wide = stream[layer, c].reshape(tc, dl).astype(F32)
        normed = (wide * gain[layer]).astype(BF16)

        def gate_tile(s, w):
            part = jnp.dot(normed, wg[layer, :, s:s + w], preferred_element_type=F32)
            part = part.reshape(ny, nx, rw, w)
            gown[:, :, :, s:s + w] = part
            gbuf[k, :, :, :, s:s + w] = part.astype(BF16)

        def up_tile(s, w):
            part = jnp.dot(normed, wu[layer, :, s:s + w], preferred_element_type=F32)
            part = part.reshape(ny, nx, rw, w)
            uown[:, :, :, s:s + w] = part
            ubuf[k, :, :, :, s:s + w] = part.astype(BF16)

        column_tiles(ff, 512, gate_tile)
        start("g1", layer, c)

        @pl.when(c == 0)
        def _():
            load_w(layer, 1).wait()

        @pl.when((layer == 0) & (c == 0))
        def _():
            load_w(0, 2).start()
            for later in range(1, layers):
                for which in range(3):
                    load_w(later, which).start()

        column_tiles(ff, 512, up_tile)
        start("u1", layer, c)
        column = jnp.sum(wide * wide, axis=1, keepdims=True)
        diagonal = lax.broadcasted_iota(jnp.int32, (tc, tc), 0) == lax.broadcasted_iota(jnp.int32, (tc, tc), 1)
        ssl[k] = jnp.broadcast_to(jnp.sum(jnp.where(diagonal, column, 0.0), axis=0, keepdims=True), (8, tc))
        start("ss", layer, c)

    def stage1(layer, c):
        k = layer * chunks + c
        arrived("g1", layer, c)
        total = gown[:, x0]
        for d in range(nx - 1):
            total = total + r1g[k, d].astype(F32)
        s1g[k] = total.astype(BF16)
        s1gown[k] = total
        start("g2", layer, c)
        arrived("u1", layer, c)
        total = uown[y0]
        for d in range(ny - 1):
            total = total + r1u[k, d].astype(F32)
        s1u[k] = total.astype(BF16)
        s1uown[k] = total
        start("u2", layer, c)

    def stage2(layer, c):
        k = layer * chunks + c
        arrived("ss", layer, c)
        squares = ssl[k, 0:1]
        for d in range(nra - 1):
            squares = squares + ssr[k, d, 0:1]
        mine = lax.broadcasted_iota(jnp.int32, (rw, tc), 0) + r * rw == lax.broadcasted_iota(jnp.int32, (rw, tc), 1)
        column = jnp.sum(jnp.where(mine, squares, 0.0), axis=1, keepdims=True)
        scale = lax.rsqrt(column / features + EPSILON)
        arrived("g2", layer, c)
        arrived("u2", layer, c)
        gate = s1gown[k, y0]
        for d in range(ny - 1):
            gate = gate + r2g[k, d].astype(F32)
        up = s1uown[k, x0]
        for d in range(nx - 1):
            up = up + r2u[k, d].astype(F32)
        hid[k, y0, x0] = (jax.nn.silu(gate * scale) * (up * scale)).astype(BF16)
        start("a1", layer, c)

    def stage3(layer, c):
        arrived("a1", layer, c)
        start("a2", layer, c)

    def stage4(layer, c):
        k = layer * chunks + c
        arrived("a2", layer, c)

        @pl.when(c == 0)
        def _():
            load_w(layer, 2).wait()

        full = hid[k].reshape(tc, ff)

        def down_tile(s, w):
            part = jnp.dot(full, wd[layer, :, s:s + w], preferred_element_type=F32)
            part = part.reshape(2, nz, rz, w)
            pown[:, :, :, s:s + w] = part
            pbuf[k, :, :, :, s:s + w] = part.astype(BF16)

        column_tiles(dl, 512, down_tile)
        start("c1", layer, c)

    def stage5(layer, c):
        k = layer * chunks + c
        arrived("c1", layer, c)
        total = pown[core] + crecv[k].astype(F32)
        csown[k] = total
        cs[k] = total.astype(BF16)
        start("z1", layer, c)

    def stage6(layer, c):
        k = layer * chunks + c
        arrived("z1", layer, c)
        branch = csown[k, z0]
        for d in range(nz - 1):
            branch = branch + zr[k, d].astype(F32)
        kept = stream[layer, c, core, z0].astype(F32)
        stream[layer + 1, c, core, z0] = (KEEP_SHARE * kept + branch).astype(BF16)
        start("z2", layer, c)

    def stage7(layer, c):
        arrived("z2", layer, c)
        start("c2", layer, c)

    def write_out(c):
        return pltpu.make_async_copy(stream.at[layers, c], out.at[c], osem.at[c])

    def stage8(layer, c):
        @pl.when(layer == layers - 1)
        def _():
            arrived("c2", layer, c)
            write_out(c).start()

    def run(stage, u, offset):
        v = u - offset
        layer, c = lax.div(v, period), lax.rem(v, period)

        @pl.when((v >= 0) & (layer < layers) & (c < chunks))
        def _():
            stage(layer, c)

    def step(u, carry):
        for stage, offset in cfg["order"]:
            run((stage0, stage1, stage2, stage3, stage4, stage5, stage6, stage7, stage8)[stage], u, offset)
        return carry

    lax.fori_loop(0, layers * period + DEPTH, step, 0)

    def finish(k, carry):
        layer, c = lax.div(k, chunks), lax.rem(k, chunks)
        for name, _ in cfg["kinds"]:
            for copy in copies(name, layer, c):
                copy.wait_send()
        return carry

    lax.fori_loop(0, layers * chunks, finish, 0)
    for c in range(chunks):
        write_out(c).wait()


ORDER = ((8, 4), (0, 0), (6, 3), (4, 2), (2, 1), (5, 2), (3, 1), (7, 3), (1, 0))


def solution(mesh):
    nra, ncb = mesh.shape["ra"], mesh.shape["cb"]
    ny = max(d for d in range(1, math.isqrt(nra) + 1) if nra % d == 0)
    nx = nra // ny
    nz = ncb // 2

    def body(tokens, norm_gain, gate_weight, up_weight, down_weight):
        rows, dl = tokens.shape
        layers, _, ff = gate_weight.shape
        tc = min(rows, max(32 * nra, 16 * ncb))
        chunks = rows // tc
        rw, rz = tc // nra, tc // ncb
        items = layers * chunks
        kinds = (("g1", nx - 1), ("u1", ny - 1), ("ss", nra - 1), ("g2", ny - 1), ("u2", nx - 1),
                 ("a1", nx + ny - 2), ("a2", nx + ny - 2), ("c1", 1), ("z1", nz - 1), ("z2", nz - 1), ("c2", 1))
        sems = sum(n for _, n in kinds)
        cfg = dict(nx=nx, ny=ny, nz=nz, layers=layers, chunks=chunks, features=dl * nra, kinds=kinds, order=ORDER)
        hbm = pl.BlockSpec(memory_space=pl.ANY)
        vmem = pl.BlockSpec(memory_space=pltpu.VMEM)
        shaped = (chunks, 2, nz, rz, dl)
        result = pl.pallas_call(
            functools.partial(kernel, cfg),
            out_shape=jax.ShapeDtypeStruct(shaped, BF16),
            in_specs=[hbm, vmem, hbm, hbm, hbm],
            out_specs=hbm,
            scratch_shapes=[
                pltpu.VMEM((layers + 1,) + shaped, BF16),
                pltpu.VMEM((layers, dl, ff), BF16),
                pltpu.VMEM((layers, dl, ff), BF16),
                pltpu.VMEM((layers, ff, dl), BF16),
                pltpu.VMEM((items, ny, nx, rw, ff), BF16),
                pltpu.VMEM((items, ny, nx, rw, ff), BF16),
                pltpu.VMEM((items, nx - 1, ny, rw, ff), BF16),
                pltpu.VMEM((items, ny - 1, nx, rw, ff), BF16),
                pltpu.VMEM((items, ny, rw, ff), BF16),
                pltpu.VMEM((items, nx, rw, ff), BF16),
                pltpu.VMEM((items, ny - 1, rw, ff), BF16),
                pltpu.VMEM((items, nx - 1, rw, ff), BF16),
                pltpu.VMEM((items, 8, tc), F32),
                pltpu.VMEM((items, nra - 1, 8, tc), F32),
                pltpu.VMEM((ny, nx, rw, ff), F32),
                pltpu.VMEM((ny, nx, rw, ff), F32),
                pltpu.VMEM((items, ny, rw, ff), F32),
                pltpu.VMEM((items, nx, rw, ff), F32),
                pltpu.VMEM((2, nz, rz, dl), F32),
                pltpu.VMEM((items, nz, rz, dl), F32),
                pltpu.VMEM((items, ny, nx, rw, ff), BF16),
                pltpu.VMEM((items, 2, nz, rz, dl), BF16),
                pltpu.VMEM((items, nz, rz, dl), BF16),
                pltpu.VMEM((items, nz, rz, dl), BF16),
                pltpu.VMEM((items, nz - 1, rz, dl), BF16),
                pltpu.SemaphoreType.DMA((layers, 3)),
                pltpu.SemaphoreType.DMA((1,)),
                pltpu.SemaphoreType.DMA((chunks,)),
                pltpu.SemaphoreType.DMA((items, sems)),
                pltpu.SemaphoreType.DMA((items, sems)),
            ],
            compiler_params=pltpu.CompilerParams(
                collective_id=0, has_side_effects=True, vmem_limit_bytes=67_043_328),
            name="sublayers",
        )(tokens.reshape(shaped), norm_gain.reshape(layers, 1, dl), gate_weight, up_weight, down_weight)
        return result.reshape(rows, dl)

    placed = (
        P(None, "ra"),
        P(None, "ra"),
        P(None, "ra", "cb"),
        P(None, "ra", "cb"),
        P(None, "cb", "ra"),
    )
    return jax.shard_map(body, mesh=mesh, in_specs=placed, out_specs=P(None, "ra"), check_vma=False)
```
